32 devices in a mesh: grp: 2 (over x), ep: 16 (over z, y, core).
Axes of the slice: x: 2, y: 2, z: 4, core: 2. Of those that a mesh axis runs over, the one named last changes fastest.
Arguments:
- resid: bfloat16 [384, 2048], P(('grp', 'ep')), parts along dimension 0, may hold values from -6 to 6
- norm_gains: float32 [4, 2048], replicated, may hold values from 0.1 to 1.9
- w_query: bfloat16 [2048, 1024], P(None, 'ep'), may hold values from -0.125 to 0.125
- w_key: bfloat16 [2048, 1024], P(None, 'ep'), may hold values from -0.125 to 0.125
- w_value: bfloat16 [2048, 1024], P(None, 'ep'), may hold values from -0.125 to 0.125
- w_outgate: bfloat16 [2048, 1024], P(None, 'ep'), may hold values from -0.125 to 0.125
- w_igate: bfloat16 [2048, 8], replicated, may hold values from -0.125 to 0.125
- w_fgate: bfloat16 [2048, 8], replicated, may hold values from -0.125 to 0.125
- igate_bias: float32 [8], replicated, may hold values from -1 to 1
- fgate_bias: float32 [8], replicated, may hold values from -1 to 5
- state_matrix: float32 [384, 8, 128, 128], P(('grp', 'ep')), parts along dimension 0, may hold values from -0.8 to 0.8
- state_norm: float32 [384, 8, 128], P(('grp', 'ep')), parts along dimension 0, may hold values from -2.4 to 2.4
- state_max: float32 [384, 8], P(('grp', 'ep')), parts along dimension 0, may hold values from -1 to 1
- w_mix_out: bfloat16 [1024, 2048], replicated, may hold values from -0.1875 to 0.1875
- routes: int32 [384, 2], P(('grp', 'ep')), parts along dimension 0, may hold values from 0 to 15, all different within a row; in each aligned block of 12 rows (0 to 11, 12 to 23, ...) at most 2 rows name the same one
- route_scores: bfloat16 [384, 2], P(('grp', 'ep')), parts along dimension 0, may hold values from 0.099609375 to 1
- expert_gate: bfloat16 [16, 2048, 512], P('ep'), may hold values from -0.125 to 0.125
- expert_up: bfloat16 [16, 2048, 512], P('ep'), may hold values from -0.125 to 0.125
- expert_down: bfloat16 [16, 512, 2048], P('ep'), may hold values from -0.25 to 0.25
- dense_gate: bfloat16 [2048, 8192], P(None, 'ep'), may hold values from -0.125 to 0.125
- dense_up: bfloat16 [2048, 8192], P(None, 'ep'), may hold values from -0.125 to 0.125
- dense_down: bfloat16 [8192, 2048], P('ep'), may hold values from -0.0625 to 0.0625
- branch_weight: bfloat16 [2048], replicated, may hold values from -0.125 to 0.125
Outputs:
- out_stream: bfloat16 [384, 2048], P(('grp', 'ep')), parts along dimension 0
- new_matrix: float32 [384, 8, 128, 128], P(('grp', 'ep')), parts along dimension 0
- new_norm: float32 [384, 8, 128], P(('grp', 'ep')), parts along dimension 0
- new_max: float32 [384, 8], P(('grp', 'ep')), parts along dimension 0
The draws below stay inside these ranges and needn't reach their ends.
There are 2 independent parts, one for each index of `grp`. The reference program is written for one: setup_inputs(seed, part) draws one part's arguments, and reference() takes and returns one part's arrays. A program takes and returns all parts, laid end to end along the dimension named above; an argument that names none is the same for every part. Nothing has to cross between parts.
Inputs may be any that keep to these rules, and one draw needn't show every extreme that they name: `routes`: each row names 2 different experts. In each aligned block of 12 rows (the rows of one device) no expert is named by more than 2 rows, a bound that some block reaches.
All inputs are finite; a program needn't handle non-finite values.
Results may differ from the reference program's by a relative error of at most 0.015.
Values may be sent and summed in bfloat16 or wider, within the bound.
A program may use at most 128 MiB of HBM per device.

```python
import math
import jax
import jax.numpy as jnp
import numpy as np
from jax import lax

D = 2048
NH = 8
DH = 128
FE = 512
FFD = 8192
TOPK = 2
SEQ_DEV = 12
INNER = 1024
CAP = 2
EXPERTS = 16
SEQS = 192
N_EP = 16


def steps_of(stream_key, shape, cuts, low, largest):
    factor_of, own = 1.0, jax.random.fold_in(stream_key, 6)
    for position, blocks in cuts:
        heights = jnp.exp(jax.random.uniform(jax.random.fold_in(own, position), (blocks,), jnp.float32, low / len(cuts), largest / len(cuts)))
        factor_of = factor_of * jnp.repeat(heights, shape[position] // blocks).reshape([-1 if axis == position else 1 for axis in range(len(shape))])
    return factor_of


def shared_out(own_key, own, number, rows, number_of, top, most, skew):
    ranking = jax.random.permutation(own_key, number_of)
    heavy_load, ordinary = portions_of(number_of, rows * top, most, skew, True), portions_of(number_of, rows * top, most, skew, False)
    places = jnp.arange(number_of)

    def named(sizes, turn):
        used = int((sizes > 0).sum())
        fixed = max(1, used // 4)
        moved = fixed + (places - fixed + turn * (used - fixed)) % max(1, number_of - fixed)
        return jnp.zeros((number_of,), jnp.int32).at[ranking[jnp.where(places < fixed, places, moved)]].set(jnp.asarray(sizes, jnp.int32))

    sizes = jnp.where(number % 4 == 0, named(heavy_load, number // 4), named(ordinary, number - number // 4 - 1))
    mixed = jax.random.permutation(jax.random.fold_in(own, 3), number_of)
    source_of, taker = mixed[0:number_of // 2 * 2:2], mixed[1:number_of // 2 * 2:2]
    slack = jnp.minimum(sizes[source_of] - 1, most - sizes[taker]) // 2
    slack = jnp.where((source_of == ranking[0]) | (taker == ranking[0]) | (sizes[taker] == 0), 0, jnp.maximum(slack, 0))
    moved = jax.random.randint(jax.random.fold_in(own, 4), (number_of // 2,), 0, 1 << 20) % (slack + 1)
    sizes = sizes.at[source_of].add(-moved).at[taker].add(moved)
    items = jnp.searchsorted(jnp.cumsum(sizes), jnp.arange(rows * top), side="right").astype(jnp.int32)
    table = items.reshape(top, rows).T
    table = table[jax.random.permutation(jax.random.fold_in(own, 1), rows)]
    turn = jax.random.randint(jax.random.fold_in(own, 2), (rows, 1), 0, top)
    return jnp.take_along_axis(table, (jnp.arange(top)[None, :] + turn) % top, axis=1)


def portions_of(number_of, total, limit, skew, full):
    loads = [(1 << 20) // math.isqrt(standing ** skew) + 1 for standing in range(1, number_of + 1)]
    largest = limit if full else min(limit, max(-(-total // number_of), total * loads[0] // sum(loads)))
    least = 1 if total - largest >= number_of - 1 else 0
    counts, spare = [largest] + [least] * (number_of - 1), total - largest - least * (number_of - 1)
    while spare > 0:
        candidates = [i for i in range(1, number_of) if counts[i] < largest] or [i for i in range(1, number_of) if counts[i] < limit]
        pool, left = sum([loads[i] for i in candidates]), spare
        for i in candidates:
            more = min(limit - counts[i], max(1, left * loads[i] // pool), spare)
            counts[i] = counts[i] + more
            spare = spare - more
    return np.array(counts)


def gaussian(rng, extent, scale, limit, cuts=(), kind=jnp.bfloat16):
    values = scale * jax.random.normal(rng, extent, jnp.float32)
    if cuts:
        values = values * steps_of(rng, extent, cuts, -0.22, 0.18)
    return jnp.clip(values, -limit, limit).astype(kind)


def setup_inputs(seed: int = 0, part: int = 0) -> dict:
    splits = jax.random.split(jax.random.key(seed), 24)
    own_keys = jax.random.split(jax.random.fold_in(splits[23], part), 24)
    resid = gaussian(own_keys[0], (SEQS, D), 1.0, 6.0, ((0, 16),))
    norm_gains = jnp.clip(1.0 + 0.18 * jax.random.normal(splits[1], (4, D), jnp.float32), 0.1, 1.9)
    w_query = gaussian(splits[2], (D, INNER), D ** -0.5, 0.125, ((1, 16),))
    w_key = gaussian(splits[3], (D, INNER), D ** -0.5, 0.125, ((1, 16),))
    w_value = gaussian(splits[4], (D, INNER), D ** -0.5, 0.125, ((1, 16),))
    w_outgate = gaussian(splits[5], (D, INNER), D ** -0.5, 0.125, ((1, 16),))
    w_igate = gaussian(splits[6], (D, NH), D ** -0.5, 0.125)
    w_fgate = gaussian(splits[7], (D, NH), D ** -0.5, 0.125)
    igate_bias = jnp.clip(jax.random.uniform(splits[8], (NH,), jnp.float32, -1.0, 1.0), -1.0, 1.0)
    fgate_bias = jnp.clip(jax.random.uniform(splits[9], (NH,), jnp.float32, -1.0, 5.0), -1.0, 5.0)
    state_matrix = gaussian(own_keys[10], (SEQS, NH, DH, DH), 0.1, 0.8, ((0, 16),), jnp.float32)
    state_norm = gaussian(own_keys[11], (SEQS, NH, DH), 0.3, 2.4, ((0, 16),), jnp.float32)
    state_max = jnp.clip(jax.random.uniform(own_keys[12], (SEQS, NH), jnp.float32, -1.0, 1.0) * steps_of(own_keys[12], (SEQS, NH), ((0, 16),), -0.4, 0.0), -1.0, 1.0)
    w_mix_out = gaussian(splits[13], (INNER, D), INNER ** -0.5, 0.1875)
    routes_keys = jax.random.split(jax.random.fold_in(own_keys[14], 1), SEQS // SEQ_DEV)
    routes_turns = jax.random.permutation(jax.random.fold_in(own_keys[14], 3), SEQS // SEQ_DEV)
    routes = jax.vmap(lambda own, number: shared_out(jax.random.fold_in(own_keys[14], 2), own, number, SEQ_DEV, EXPERTS, TOPK, CAP, 2))(routes_keys, routes_turns).reshape((SEQS, TOPK))
    route_scores = jnp.clip(jnp.exp(math.log(1.0) - 2.306499 * jax.random.uniform(own_keys[15], (SEQS, TOPK), jnp.float32) ** steps_of(own_keys[15], (SEQS, TOPK), ((0, 16),), -0.2, 0.2)), 0.099609375, 1.0).astype(jnp.bfloat16)
    expert_gate = gaussian(splits[16], (EXPERTS, D, FE), D ** -0.5, 0.125, ((0, 16),))
    expert_up = gaussian(splits[17], (EXPERTS, D, FE), D ** -0.5, 0.125, ((0, 16),))
    expert_down = gaussian(splits[18], (EXPERTS, FE, D), FE ** -0.5, 0.25, ((0, 16),))
    dense_gate = gaussian(splits[19], (D, FFD), D ** -0.5, 0.125, ((1, 16),))
    dense_up = gaussian(splits[20], (D, FFD), D ** -0.5, 0.125, ((1, 16),))
    dense_down = gaussian(splits[21], (FFD, D), FFD ** -0.5, 0.0625, ((0, 16),))
    branch_weight = gaussian(splits[22], (D,), D ** -0.5, 0.125)
    return {"resid": resid, "norm_gains": norm_gains, "w_query": w_query, "w_key": w_key, "w_value": w_value, "w_outgate": w_outgate, "w_igate": w_igate, "w_fgate": w_fgate, "igate_bias": igate_bias, "fgate_bias": fgate_bias, "state_matrix": state_matrix, "state_norm": state_norm, "state_max": state_max, "w_mix_out": w_mix_out, "routes": routes, "route_scores": route_scores, "expert_gate": expert_gate, "expert_up": expert_up, "expert_down": expert_down, "dense_gate": dense_gate, "dense_up": dense_up, "dense_down": dense_down, "branch_weight": branch_weight}


def rms_scale(values, gains):
    return values * lax.rsqrt(lax.optimization_barrier(jnp.mean(values * values, axis=-1, keepdims=True)) + 1e-06) * gains.astype(jnp.float32)

def round_half(values):
    return lax.optimization_barrier(values.astype(jnp.bfloat16)).astype(jnp.float32)

def expert_ffn(picked, gate_matrix, up_matrix, down_matrix):
    gate_out = jnp.dot(picked, gate_matrix, preferred_element_type=jnp.float32)
    up_out = jnp.dot(picked, up_matrix, preferred_element_type=jnp.float32)
    hidden = (jax.nn.silu(gate_out) * up_out).astype(jnp.bfloat16)
    return jnp.dot(hidden, down_matrix, preferred_element_type=jnp.float32).astype(jnp.bfloat16)

def expert_mix(branch_in, routes, route_scores, expert_gate, expert_up, expert_down):
    tokens = branch_in.shape[0]
    experts = expert_gate.shape[0]
    onehot = (routes[:, :, None] == jnp.arange(experts, dtype=jnp.int32)[None, None, :]).astype(jnp.float32)
    scores = route_scores.astype(jnp.float32)
    shares = scores / lax.optimization_barrier(jnp.sum(scores, axis=-1, keepdims=True))
    weights = lax.optimization_barrier(jnp.sum(shares[:, :, None] * onehot, axis=1))
    hit_count = lax.optimization_barrier(jnp.sum(onehot, axis=1))
    hit_int = hit_count.astype(jnp.int32).reshape(N_EP, SEQ_DEV, experts)
    rank_index = jnp.cumsum(hit_int, axis=1) - hit_int
    block_base = (jnp.arange(N_EP, dtype=jnp.int32) * CAP)[:, None, None]
    slot_index = (rank_index + block_base).reshape(tokens, experts).T
    hit_flags = hit_count.T
    weight_rows = weights.T
    slot_range = jnp.arange(N_EP * CAP, dtype=jnp.int32)

    def expert_step(running_sum, expert_index):
        chosen = ((slot_index[expert_index][None, :] == slot_range[:, None]) & (hit_flags[expert_index][None, :] > 0.5)).astype(jnp.float32)
        picked = jnp.dot(chosen.astype(jnp.bfloat16), branch_in, preferred_element_type=jnp.float32).astype(jnp.bfloat16)
        produced = expert_ffn(picked, expert_gate[expert_index], expert_up[expert_index], expert_down[expert_index])
        weighted = chosen * weight_rows[expert_index][None, :]
        contribution = jnp.dot(weighted.T, produced.astype(jnp.float32), precision=lax.Precision.HIGHEST)
        running_sum = running_sum + round_half(contribution)
        return (running_sum, None)
    start_sum = jnp.zeros(branch_in.shape, jnp.float32)
    result, ignored = lax.scan(expert_step, start_sum, jnp.arange(experts, dtype=jnp.int32))
    return result

def reference(resid, norm_gains, w_query, w_key, w_value, w_outgate, w_igate, w_fgate, igate_bias, fgate_bias, state_matrix, state_norm, state_max, w_mix_out, routes, route_scores, expert_gate, expert_up, expert_down, dense_gate, dense_up, dense_down, branch_weight):
    seqs = resid.shape[0]
    heads = state_matrix.shape[1]
    head_size = state_matrix.shape[2]
    resid32 = resid.astype(jnp.float32)
    normed = rms_scale(resid32, norm_gains[0]).astype(jnp.bfloat16)

    def project(matrix):
        result = jnp.dot(normed, matrix, preferred_element_type=jnp.float32).astype(jnp.bfloat16)
        return result.astype(jnp.float32).reshape(seqs, heads, head_size)
    query = project(w_query)
    key_heads = project(w_key) * head_size ** (-0.5)
    value_heads = project(w_value)
    outgate = project(w_outgate)
    ipre = jnp.dot(normed, w_igate, preferred_element_type=jnp.float32) + igate_bias
    fpre = jnp.dot(normed, w_fgate, preferred_element_type=jnp.float32) + fgate_bias
    logf = jax.nn.log_sigmoid(fpre)
    new_max = jnp.maximum(ipre, logf + state_max)
    keep_gain = jnp.exp(logf + state_max - new_max)
    write_gain = jnp.exp(ipre - new_max)
    new_matrix = keep_gain[:, :, None, None] * state_matrix + write_gain[:, :, None, None] * value_heads[:, :, :, None] * key_heads[:, :, None, :]
    new_norm = keep_gain[:, :, None] * state_norm + write_gain[:, :, None] * key_heads
    numer = jnp.einsum('shed,shd->she', new_matrix, query, precision=lax.Precision.HIGHEST)
    denom = lax.optimization_barrier(jnp.sum(new_norm * query, axis=-1))
    cell = numer / jnp.maximum(jnp.abs(denom), 1.0)[:, :, None]
    gated = (jax.nn.sigmoid(outgate) * cell).reshape(seqs, heads * head_size).astype(jnp.bfloat16)
    mixed = jnp.dot(gated, w_mix_out, preferred_element_type=jnp.float32)
    middle = resid32 + rms_scale(mixed, norm_gains[1])
    branch_in = rms_scale(middle, norm_gains[2]).astype(jnp.bfloat16)
    moe = expert_mix(branch_in, routes, route_scores, expert_gate, expert_up, expert_down)
    gate_out = jnp.dot(branch_in, dense_gate, preferred_element_type=jnp.float32)
    up_out = jnp.dot(branch_in, dense_up, preferred_element_type=jnp.float32)
    hidden = (jax.nn.silu(gate_out) * up_out).astype(jnp.bfloat16)
    logit = jnp.dot(branch_in, branch_weight, preferred_element_type=jnp.float32)
    branch_gate = jax.nn.sigmoid(logit)[:, None]
    block_width = hidden.shape[1] // N_EP
    hidden_blocks = jnp.transpose(hidden.reshape(seqs, N_EP, block_width), (1, 0, 2))
    down_blocks = dense_down.reshape(N_EP, block_width, dense_down.shape[1])

    def dense_step(running_sum, pieces):
        hidden_block, down_block = pieces
        term = jnp.dot(hidden_block, down_block, preferred_element_type=jnp.float32) * branch_gate
        return (running_sum + round_half(term), None)
    dense, ignored = lax.scan(dense_step, jnp.zeros(middle.shape, jnp.float32), (hidden_blocks, down_blocks))
    combined = moe + dense
    out_stream = (middle + rms_scale(combined, norm_gains[3])).astype(jnp.bfloat16)
    return (out_stream, new_matrix, new_norm, new_max)
```

```python
import functools

import jax
import jax.numpy as jnp
from jax import lax
from jax.experimental import pallas as pl
from jax.experimental.pallas import tpu as pltpu
from jax.sharding import PartitionSpec as P

MESH = pl.DeviceIdType.MESH
F32 = jnp.float32
BF16 = jnp.bfloat16
ROWS = 16
TABLE = 128
CHUNKS = 4


def rms_scale(values, gains):
    return values * lax.rsqrt(jnp.mean(values * values, axis=-1, keepdims=True) + 1e-06) * gains


def place():
    me = lax.axis_index("ep")
    return lax.div(me, 4), lax.rem(lax.div(me, 2), 2), lax.rem(me, 2)


def device(a, b, c):
    return {"ep": (a * 2 + b) * 2 + c}


def near_first(count):
    return sorted(range(1, count), key=lambda k: (min(k, count - k), k))


def push(src, dst, send_sem, recv_sem, to):
    copy = pltpu.make_async_remote_copy(
        src_ref=src, dst_ref=dst, send_sem=send_sem, recv_sem=recv_sem,
        device_id=to, device_id_type=MESH,
    )
    copy.start()
    return copy


def arrived(dst, send_sem, recv_sem, to):
    pltpu.make_async_remote_copy(
        src_ref=dst, dst_ref=dst, send_sem=send_sem, recv_sem=recv_sem,
        device_id=to, device_id_type=MESH,
    ).wait_recv()


def gather(buf, a, b, c, groups, send_z, send_y, send_d, recv):
    order = near_first(groups)
    y_peer, d_peer = device(a, 1 - b, c), device(a, b, 1 - c)
    sent = []

    def send(bb, aa, to, sem):
        block = buf.at[c, bb, aa]
        sent.append(push(block, block, sem, recv.at[c, bb, aa], to))

    def wait(cc, bb, aa):
        arrived(buf.at[cc, bb, aa], send_d.at[0, 0], recv.at[cc, bb, aa], d_peer)

    for k in order:
        send(b, a, device(lax.rem(a + k, groups), b, c), send_z.at[k])
    send(b, a, y_peer, send_y.at[0])
    send(b, a, d_peer, send_d.at[0, 0])
    for k in order:
        src = lax.rem(a + k, groups)
        wait(c, b, src)
        send(b, src, y_peer, send_y.at[k])
        send(b, src, d_peer, send_d.at[0, k])
    for k in [0] + order:
        src = lax.rem(a + k, groups)
        wait(c, 1 - b, src)
        send(1 - b, src, d_peer, send_d.at[1, k])
    for bb in range(2):
        for aa in range(groups):
            wait(1 - c, bb, aa)
    for copy in sent:
        copy.wait_send()


def project_kernel(
    n, resid_ref, gain_ref, wq_ref, wk_ref, wv_ref, wo_ref, out_ref,
    rows, local, landed, send_z, send_y, send_d, recv, send_x, recv_x,
):
    groups = n // 4
    a, b, c = place()
    me = lax.axis_index("ep")
    rows_local = resid_ref.shape[0]
    width = wq_ref.shape[1]
    barrier = pltpu.get_barrier_semaphore()
    for k in range(1, n):
        pl.semaphore_signal(
            barrier, inc=1, device_id={"ep": lax.rem(me + k, n)}, device_id_type=MESH
        )
    normed = rms_scale(resid_ref[...].astype(F32), gain_ref[...]).astype(BF16)
    rows[c, b, a] = jnp.zeros(rows.shape[3:], BF16)
    rows[c, b, a, 0:rows_local, :] = normed
    pl.semaphore_wait(barrier, n - 1)
    gather(rows, a, b, c, groups, send_z, send_y, send_d, recv)
    everything = rows[...].reshape(n * ROWS, rows.shape[-1])
    for m, w_ref in enumerate((wq_ref, wk_ref, wv_ref, wo_ref)):
        piece = jnp.dot(everything, w_ref[...], preferred_element_type=F32).astype(BF16)
        local[:, :, :, :, m * width : (m + 1) * width] = piece.reshape(2, 2, groups, ROWS, width)
    sent = []
    for k in range(1, n):
        to = lax.rem(me + k, n)
        block = local.at[lax.rem(to, 2), lax.rem(lax.div(to, 2), 2), lax.div(to, 4)]
        sent.append(push(block, landed.at[c, b, a], send_x.at[k], recv_x.at[c, b, a], {"ep": to}))
    landed[c, b, a] = local[c, b, a]
    for k in range(1, n):
        src = lax.rem(me + k, n)
        cc, bb, aa = lax.rem(src, 2), lax.rem(lax.div(src, 2), 2), lax.div(src, 4)
        arrived(landed.at[cc, bb, aa], send_x.at[k], recv_x.at[cc, bb, aa], {"ep": src})
    for aa in range(groups):
        for bb in range(2):
            for cc in range(2):
                start = ((aa * 2 + bb) * 2 + cc) * width
                for m in range(4):
                    out_ref[m, :, start : start + width] = landed[
                        cc, bb, aa, :, m * width : (m + 1) * width
                    ]
    for copy in sent:
        copy.wait_send()


def project(resid, gain, weights, n):
    rows_local, d = resid.shape
    width = weights[0].shape[1]
    groups = n // 4
    vmem = pl.BlockSpec(memory_space=pltpu.VMEM)
    return pl.pallas_call(
        functools.partial(project_kernel, n),
        out_shape=jax.ShapeDtypeStruct((4, ROWS, n * width), BF16),
        in_specs=[vmem] * 6,
        out_specs=vmem,
        scratch_shapes=[
            pltpu.VMEM((2, 2, groups, ROWS, d), BF16),
            pltpu.VMEM((2, 2, groups, ROWS, 4 * width), BF16),
            pltpu.VMEM((2, 2, groups, ROWS, 4 * width), BF16),
            pltpu.SemaphoreType.DMA((groups,)),
            pltpu.SemaphoreType.DMA((groups,)),
            pltpu.SemaphoreType.DMA((2, groups)),
            pltpu.SemaphoreType.DMA((2, 2, groups)),
            pltpu.SemaphoreType.DMA((n,)),
            pltpu.SemaphoreType.DMA((2, 2, groups)),
        ],
        compiler_params=pltpu.CompilerParams(
            collective_id=0, has_side_effects=True, vmem_limit_bytes=32 * 2**20
        ),
        name="project",
    )(resid, gain, *weights)


def branch_kernel(
    n, branch_ref, table_ref, middle_ref, gain_ref, gate_w_ref,
    eg_hbm, eu_hbm, ed_hbm, dg_hbm, du_hbm, dd_hbm, out_ref,
    rows, eg, eu, ed, dg, du, dd, hid_e, hid_d,
    term, recv1, part1, recv2, part2, recv3,
    load, send_z, send_y, send_d, recv, s1, r1, s2, r2, s3, r3,
):
    groups = n // 4
    a, b, c = place()
    me = lax.axis_index("ep")
    rows_local, d = branch_ref.shape
    experts_local = eg.shape[0]
    order = near_first(groups)
    y_peer, d_peer = device(a, 1 - b, c), device(a, b, 1 - c)
    barrier = pltpu.get_barrier_semaphore()
    for to in [device(lax.rem(a + k, groups), b, c) for k in order] + [y_peer, d_peer]:
        pl.semaphore_signal(barrier, inc=1, device_id=to, device_id_type=MESH)
    loads = []
    for i, (src, dst) in enumerate(
        ((dg_hbm, dg), (du_hbm, du), (eg_hbm, eg), (eu_hbm, eu), (dd_hbm, dd), (ed_hbm, ed))
    ):
        loads.append(pltpu.make_async_copy(src, dst, load.at[i]))
        loads[-1].start()
    rows[c, b, a] = jnp.zeros(rows.shape[3:], BF16)
    rows[c, b, a, 0:rows_local, 0:d] = branch_ref[...]
    rows[c, b, a, 0:rows_local, d : d + TABLE] = table_ref[...]
    pl.semaphore_wait(barrier, groups + 1)
    gather(rows, a, b, c, groups, send_z, send_y, send_d, recv)
    for copy in loads:
        copy.wait()

    everything = rows[:, :, :, :, 0:d].reshape(n * ROWS, d)
    table = rows[:, :, :, :, d : d + TABLE].reshape(n * ROWS, TABLE).astype(F32)
    total = jnp.sum(table, axis=-1, keepdims=True)
    total = jnp.where(total > 0.0, total, 1.0)
    lanes = lax.broadcasted_iota(jnp.int32, table.shape, 1)
    logit = jnp.sum(everything.astype(F32) * gate_w_ref[...].astype(F32), axis=-1, keepdims=True)
    branch_gate = jax.nn.sigmoid(logit)

    def ffn(gate, up, hid, wide):
        step = min(256, wide)
        for j in range(wide // step):
            cols = slice(j * step, (j + 1) * step)
            g = jnp.dot(everything, gate[:, cols], preferred_element_type=F32)
            u = jnp.dot(everything, up[:, cols], preferred_element_type=F32)
            hid[:, cols] = (jax.nn.silu(g) * u).astype(BF16)

    ffn(dg, du, hid_d, dg.shape[1])
    shares = []
    for e in range(experts_local):
        ffn(eg.at[e], eu.at[e], hid_e.at[e], eg.shape[2])
        mine = jnp.sum(jnp.where(lanes == me * experts_local + e, table, 0.0), axis=-1, keepdims=True)
        shares.append(mine / total)

    wide = d // CHUNKS
    copies = []
    for h in range(CHUNKS):
        cols = slice(h * wide, (h + 1) * wide)
        value = (jnp.dot(hid_d[...], dd[:, cols], preferred_element_type=F32) * branch_gate).astype(BF16).astype(F32)
        for e in range(experts_local):
            y = jnp.dot(hid_e[e], ed[e, :, cols], preferred_element_type=F32).astype(BF16).astype(F32)
            value = value + (shares[e] * y).astype(BF16).astype(F32)
        term[h] = value.astype(BF16).reshape(2, 2, groups, ROWS, wide)
        copies.append(push(term.at[h, 1 - c], recv1.at[h], s1.at[h], r1.at[h], d_peer))
    for h in range(CHUNKS):
        copies[h].wait_recv()
        part1[h] = (term[h, c].astype(F32) + recv1[h].astype(F32)).astype(BF16)
        copies.append(push(part1.at[h, 1 - b], recv2.at[h], s2.at[h], r2.at[h], y_peer))
    for h in range(CHUNKS):
        copies[CHUNKS + h].wait_recv()
        part2[h] = (part1[h, b].astype(F32) + recv2[h].astype(F32)).astype(BF16)
        for k in order:
            to = lax.rem(a + k, groups)
            copies.append(
                push(part2.at[h, to], recv3.at[h, a], s3.at[h, k], r3.at[h, a], device(to, b, c))
            )
    sums, square = [], 0.0
    for h in range(CHUNKS):
        value = part2[h, a].astype(F32)
        for k in order:
            src = lax.rem(a + k, groups)
            arrived(recv3.at[h, src], s3.at[h, k], r3.at[h, src], device(src, b, c))
            value = value + recv3[h, src].astype(F32)
        sums.append(value)
        square = square + jnp.sum(value * value, axis=-1, keepdims=True)
    scale = lax.rsqrt(square / d + 1e-06)
    for h in range(CHUNKS):
        cols = slice(h * wide, (h + 1) * wide)
        extra = (sums[h] * scale * gain_ref[:, cols])[0:rows_local]
        out_ref[:, cols] = (middle_ref[:, cols] + extra).astype(BF16)
    for copy in copies:
        copy.wait_send()


def branches(branch_in, table, middle, gain, gate_w, experts, dense, n):
    rows_local, d = branch_in.shape
    groups = n // 4
    vmem = pl.BlockSpec(memory_space=pltpu.VMEM)
    hbm = pl.BlockSpec(memory_space=pl.ANY)
    wide = d // CHUNKS
    dma = pltpu.SemaphoreType.DMA
    return pl.pallas_call(
        functools.partial(branch_kernel, n),
        out_shape=jax.ShapeDtypeStruct((rows_local, d), BF16),
        in_specs=[vmem] * 5 + [hbm] * 6,
        out_specs=vmem,
        scratch_shapes=[
            pltpu.VMEM((2, 2, groups, ROWS, d + TABLE), BF16),
            *[pltpu.VMEM(w.shape, BF16) for w in experts],
            *[pltpu.VMEM(w.shape, BF16) for w in dense],
            pltpu.VMEM((experts[0].shape[0], n * ROWS, experts[0].shape[2]), BF16),
            pltpu.VMEM((n * ROWS, dense[0].shape[1]), BF16),
            pltpu.VMEM((CHUNKS, 2, 2, groups, ROWS, wide), BF16),
            pltpu.VMEM((CHUNKS, 2, groups, ROWS, wide), BF16),
            pltpu.VMEM((CHUNKS, 2, groups, ROWS, wide), BF16),
            pltpu.VMEM((CHUNKS, groups, ROWS, wide), BF16),
            pltpu.VMEM((CHUNKS, groups, ROWS, wide), BF16),
            pltpu.VMEM((CHUNKS, groups, ROWS, wide), BF16),
            dma((6,)),
            dma((groups,)),
            dma((groups,)),
            dma((2, groups)),
            dma((2, 2, groups)),
            dma((CHUNKS,)),
            dma((CHUNKS,)),
            dma((CHUNKS,)),
            dma((CHUNKS,)),
            dma((CHUNKS, groups)),
            dma((CHUNKS, groups)),
        ],
        compiler_params=pltpu.CompilerParams(
            collective_id=1, has_side_effects=True, vmem_limit_bytes=48 * 2**20
        ),
        name="branches",
    )(branch_in, table, middle, gain, gate_w, *experts, *dense)


def local(
    resid, norm_gains, w_query, w_key, w_value, w_outgate, w_igate, w_fgate,
    igate_bias, fgate_bias, state_matrix, state_norm, state_max, w_mix_out,
    routes, route_scores, expert_gate, expert_up, expert_down,
    dense_gate, dense_up, dense_down, branch_weight,
):
    seqs_local = resid.shape[0]
    heads = state_matrix.shape[1]
    head_size = state_matrix.shape[2]
    devices_ep = lax.axis_size("ep")
    resid32 = resid.astype(F32)
    own_proj = project(
        resid, norm_gains[0:1], (w_query, w_key, w_value, w_outgate), devices_ep
    )[:, :seqs_local]
    normed = rms_scale(resid32, norm_gains[0]).astype(BF16)
    head_shape = (seqs_local, heads, head_size)
    query = own_proj[0].astype(F32).reshape(head_shape)
    key_heads = own_proj[1].astype(F32).reshape(head_shape) * head_size ** (-0.5)
    value_heads = own_proj[2].astype(F32).reshape(head_shape)
    outgate = own_proj[3].astype(F32).reshape(head_shape)
    ipre = jnp.dot(normed, w_igate, preferred_element_type=F32) + igate_bias
    fpre = jnp.dot(normed, w_fgate, preferred_element_type=F32) + fgate_bias
    logf = jax.nn.log_sigmoid(fpre)
    new_max = jnp.maximum(ipre, logf + state_max)
    keep_gain = jnp.exp(logf + state_max - new_max)
    write_gain = jnp.exp(ipre - new_max)
    new_matrix = (
        keep_gain[:, :, None, None] * state_matrix
        + write_gain[:, :, None, None] * value_heads[:, :, :, None] * key_heads[:, :, None, :]
    )
    new_norm = keep_gain[:, :, None] * state_norm + write_gain[:, :, None] * key_heads
    numer = jnp.einsum("shed,shd->she", new_matrix, query, precision=lax.Precision.HIGHEST)
    denom = jnp.sum(new_norm * query, axis=-1)
    cell = numer / jnp.maximum(jnp.abs(denom), 1.0)[:, :, None]
    gated = (
        (jax.nn.sigmoid(outgate) * cell).reshape(seqs_local, heads * head_size).astype(BF16)
    )
    mixed = jnp.dot(gated, w_mix_out, preferred_element_type=F32)
    middle = resid32 + rms_scale(mixed, norm_gains[1])
    branch_in = rms_scale(middle, norm_gains[2]).astype(BF16)
    lanes = jnp.arange(TABLE, dtype=jnp.int32)
    table = jnp.sum(
        jnp.where(routes[:, :, None] == lanes, route_scores.astype(F32)[:, :, None], 0.0), axis=1
    ).astype(BF16)
    out_stream = branches(
        branch_in, table, middle, norm_gains[3:4], branch_weight[None],
        (expert_gate, expert_up, expert_down), (dense_gate, dense_up, dense_down), devices_ep,
    )
    return (out_stream, new_matrix, new_norm, new_max)


def solution(mesh):
    rows = ("grp", "ep")
    placed = (
        P(rows, None),
        P(),
        P(None, "ep"),
        P(None, "ep"),
        P(None, "ep"),
        P(None, "ep"),
        P(),
        P(),
        P(),
        P(),
        P(rows, None, None, None),
        P(rows, None, None),
        P(rows, None),
        P(),
        P(rows, None),
        P(rows, None),
        P("ep", None, None),
        P("ep", None, None),
        P("ep", None, None),
        P(None, "ep"),
        P(None, "ep"),
        P("ep", None),
        P(),
    )
    return jax.shard_map(
        local,
        mesh=mesh,
        in_specs=placed,
        out_specs=(
            P(rows, None),
            P(rows, None, None, None),
            P(rows, None, None),
            P(rows, None),
        ),
        check_vma=False,
    )
```

```python
import functools

import jax
import jax.numpy as jnp
from jax import lax
from jax.experimental import pallas as pl
from jax.experimental.pallas import tpu as pltpu
from jax.sharding import PartitionSpec as P

MESH = pl.DeviceIdType.MESH
F32 = jnp.float32
BF16 = jnp.bfloat16
ROWS = 16
TABLE = 128
VMEM_BYTES = 61 * 2**20
CHUNKS = 4


def rms_scale(values, gains):
    return values * lax.rsqrt(jnp.mean(values * values, axis=-1, keepdims=True) + 1e-06) * gains


def spent(us):
    return pl.CostEstimate(flops=us * 10**9, bytes_accessed=us * 2 * 10**6, transcendentals=0)


def dot_t(left, right):
    return lax.dot_general(left, right, (((1,), (1,)), ((), ())), preferred_element_type=F32)


def place():
    me = lax.axis_index("ep")
    return lax.div(me, 4), lax.rem(lax.div(me, 2), 2), lax.rem(me, 2)


def device(a, b, c):
    return {"ep": (a * 2 + b) * 2 + c}


def near_first(count):
    return sorted(range(1, count), key=lambda k: (min(k, count - k), k))


def push(src, dst, send_sem, recv_sem, to):
    copy = pltpu.make_async_remote_copy(
        src_ref=src, dst_ref=dst, send_sem=send_sem, recv_sem=recv_sem,
        device_id=to, device_id_type=MESH,
    )
    copy.start()
    return copy


def arrived(dst, send_sem, recv_sem, to):
    pltpu.make_async_remote_copy(
        src_ref=dst, dst_ref=dst, send_sem=send_sem, recv_sem=recv_sem,
        device_id=to, device_id_type=MESH,
    ).wait_recv()


def gather(buf, a, b, c, groups, send_z, send_y, send_d, recv):
    order = near_first(groups)
    y_peer, d_peer = device(a, 1 - b, c), device(a, b, 1 - c)
    sent = []

    def send(bb, aa, to, sem):
        block = buf.at[c, bb, aa]
        sent.append(push(block, block, sem, recv.at[c, bb, aa], to))

    def wait(cc, bb, aa):
        arrived(buf.at[cc, bb, aa], send_d.at[0, 0], recv.at[cc, bb, aa], d_peer)

    for k in order:
        send(b, a, device(lax.rem(a + k, groups), b, c), send_z.at[k])
    send(b, a, y_peer, send_y.at[0])
    send(b, a, d_peer, send_d.at[0, 0])
    for k in order:
        src = lax.rem(a + k, groups)
        wait(c, b, src)
        send(b, src, y_peer, send_y.at[k])
        send(b, src, d_peer, send_d.at[0, k])
    for k in [0] + order:
        src = lax.rem(a + k, groups)
        wait(c, 1 - b, src)
        send(1 - b, src, d_peer, send_d.at[1, k])
    for bb in range(2):
        for aa in range(groups):
            wait(1 - c, bb, aa)
    for copy in sent:
        copy.wait_send()


def project_kernel(
    n, resid_ref, gain_ref, wq_ref, wk_ref, wv_ref, wo_ref, out_ref,
    wq, wk, wv, wo, rows, local, landed, load, send_z, send_y, send_d, recv, send_x, recv_x,
):
    groups = n // 4
    a, b, c = place()
    me = lax.axis_index("ep")
    rows_local = resid_ref.shape[0]
    width = wq.shape[0]
    barrier = pltpu.get_barrier_semaphore()
    for k in range(1, n):
        pl.semaphore_signal(
            barrier, inc=1, device_id={"ep": lax.rem(me + k, n)}, device_id_type=MESH
        )
    loads = [
        pltpu.make_async_copy(src, dst, load.at[i])
        for i, (src, dst) in enumerate(((wq_ref, wq), (wk_ref, wk), (wv_ref, wv), (wo_ref, wo)))
    ]
    for copy in loads:
        copy.start()
    normed = rms_scale(resid_ref[...].astype(F32), gain_ref[...]).astype(BF16)
    rows[c, b, a] = jnp.zeros(rows.shape[3:], BF16)
    rows[c, b, a, 0:rows_local, :] = normed
    pl.semaphore_wait(barrier, n - 1)
    gather(rows, a, b, c, groups, send_z, send_y, send_d, recv)
    everything = rows[...].reshape(n * ROWS, rows.shape[-1])
    for copy in loads:
        copy.wait()
    for m, w_ref in enumerate((wq, wk, wv, wo)):
        piece = dot_t(everything, w_ref[...]).astype(BF16)
        local[:, :, :, :, m * width : (m + 1) * width] = piece.reshape(2, 2, groups, ROWS, width)
    sent = []
    for k in range(1, n):
        to = lax.rem(me + k, n)
        block = local.at[lax.rem(to, 2), lax.rem(lax.div(to, 2), 2), lax.div(to, 4)]
        sent.append(push(block, landed.at[c, b, a], send_x.at[k], recv_x.at[c, b, a], {"ep": to}))
    landed[c, b, a] = local[c, b, a]
    for k in range(1, n):
        src = lax.rem(me + k, n)
        cc, bb, aa = lax.rem(src, 2), lax.rem(lax.div(src, 2), 2), lax.div(src, 4)
        arrived(landed.at[cc, bb, aa], send_x.at[k], recv_x.at[cc, bb, aa], {"ep": src})
    for aa in range(groups):
        for bb in range(2):
            for cc in range(2):
                start = ((aa * 2 + bb) * 2 + cc) * width
                for m in range(4):
                    out_ref[m, :, start : start + width] = landed[
                        cc, bb, aa, :, m * width : (m + 1) * width
                    ]
    for copy in sent:
        copy.wait_send()


def project(resid, gain, weights, n):
    rows_local, d = resid.shape
    width = weights[0].shape[0]
    groups = n // 4
    vmem = pl.BlockSpec(memory_space=pltpu.VMEM)
    return pl.pallas_call(
        functools.partial(project_kernel, n),
        out_shape=jax.ShapeDtypeStruct((4, ROWS, n * width), BF16),
        in_specs=[vmem] * 2 + [pl.BlockSpec(memory_space=pltpu.HBM)] * 4,
        out_specs=vmem,
        scratch_shapes=[
            *[pltpu.VMEM(w.shape, BF16) for w in weights],
            pltpu.VMEM((2, 2, groups, ROWS, d), BF16),
            pltpu.VMEM((2, 2, groups, ROWS, 4 * width), BF16),
            pltpu.VMEM((2, 2, groups, ROWS, 4 * width), BF16),
            pltpu.SemaphoreType.DMA((4,)),
            pltpu.SemaphoreType.DMA((groups,)),
            pltpu.SemaphoreType.DMA((groups,)),
            pltpu.SemaphoreType.DMA((2, groups)),
            pltpu.SemaphoreType.DMA((2, 2, groups)),
            pltpu.SemaphoreType.DMA((n,)),
            pltpu.SemaphoreType.DMA((2, 2, groups)),
        ],
        compiler_params=pltpu.CompilerParams(
            collective_id=0, has_side_effects=True, vmem_limit_bytes=VMEM_BYTES
        ),
        cost_estimate=spent(20),
        name="project",
    )(resid, gain, *weights)


def cell_kernel(
    proj_ref, resid_ref, gain_ref, wi_ref, wf_ref, bi_ref, bf_ref, max_ref, norm_ref, state_hbm,
    matrix_hbm, norm_out, max_out, gated_ref,
    old, fresh, q3, k3, wv3, keep3, numer3, load, sem,
):
    count, heads, size, _ = old.shape

    def loading(s):
        return pltpu.make_async_copy(state_hbm.at[s], old.at[s], load.at[s])

    for s in range(count):
        loading(s).start()
    normed = rms_scale(resid_ref[...].astype(F32), gain_ref[...]).astype(BF16)
    ipre = dot_t(normed, wi_ref[...]) + bi_ref[...]
    fpre = dot_t(normed, wf_ref[...]) + bf_ref[...]
    logf = jnp.minimum(fpre, 0.0) - jnp.log1p(jnp.exp(-jnp.abs(fpre)))
    old_max = logf + max_ref[...]
    new_max = jnp.maximum(ipre, old_max)
    max_out[...] = new_max
    keep = jnp.exp(old_max - new_max)
    write = jnp.exp(ipre - new_max)
    denoms = []
    for h in range(heads):
        cols = slice(h * size, (h + 1) * size)
        q = proj_ref[0, 0:count, cols].astype(F32)
        k = proj_ref[1, 0:count, cols].astype(F32) * size ** (-0.5)
        v = proj_ref[2, 0:count, cols].astype(F32)
        keep_h, write_h = keep[:, h : h + 1], write[:, h : h + 1]
        new_norm = keep_h * norm_ref[:, h, :] + write_h * k
        norm_out[:, h, :] = new_norm
        denoms.append(jnp.maximum(jnp.abs(jnp.sum(new_norm * q, axis=-1, keepdims=True)), 1.0))
        q3[:, h, :] = q
        k3[:, h, :] = k
        wv3[:, h, :] = write_h * v
        keep3[:, h, :] = jnp.broadcast_to(keep_h, (count, size))

    def sequence(s, carry):
        q, k, kept = q3[s], k3[s], keep3[s]
        loading(s).wait()
        column = wv3[s].T
        lane = lax.broadcasted_iota(jnp.int32, (size, heads), 1)
        numer = jnp.zeros((size, heads), F32)
        for h in range(heads):
            new = (
                old[s, h] * kept[h : h + 1, :] + column[:, h : h + 1] * k[h : h + 1, :]
            )
            fresh[s, h] = new
            read = jnp.sum(new * q[h : h + 1, :], axis=-1, keepdims=True)
            numer = jnp.where(lane == h, read, numer)
        pltpu.make_async_copy(fresh.at[s], matrix_hbm.at[s], sem.at[s]).start()
        numer3[s] = numer.T
        return carry

    lax.fori_loop(0, count, sequence, 0)
    for h in range(heads):
        cols = slice(h * size, (h + 1) * size)
        outgate = proj_ref[3, 0:count, cols].astype(F32)
        cell = numer3[:, h, :] / denoms[h]
        gated_ref[:, cols] = (jax.nn.sigmoid(outgate) * cell).astype(BF16)
    for s in range(count):
        pltpu.make_async_copy(fresh.at[s], matrix_hbm.at[s], sem.at[s]).wait()


def cell_update(proj, resid, gain, gates, biases, state_max, state_norm, state):
    count, heads, size, _ = state.shape
    vmem = pl.BlockSpec(memory_space=pltpu.VMEM)
    small = pltpu.VMEM((count, heads, size), F32)
    return pl.pallas_call(
        cell_kernel,
        out_shape=(
            jax.ShapeDtypeStruct(state.shape, F32),
            jax.ShapeDtypeStruct(state_norm.shape, F32),
            jax.ShapeDtypeStruct(state_max.shape, F32),
            jax.ShapeDtypeStruct((count, heads * size), BF16),
        ),
        in_specs=[vmem] * 9 + [pl.BlockSpec(memory_space=pl.ANY)],
        out_specs=(pl.BlockSpec(memory_space=pl.ANY), vmem, vmem, vmem),
        scratch_shapes=[
            pltpu.VMEM(state.shape, F32),
            pltpu.VMEM(state.shape, F32),
            small, small, small, small, small,
            pltpu.SemaphoreType.DMA((count,)),
            pltpu.SemaphoreType.DMA((count,)),
        ],
        compiler_params=pltpu.CompilerParams(vmem_limit_bytes=VMEM_BYTES),
        cost_estimate=spent(6),
        name="cell_update",
    )(proj, resid, gain, *gates, *biases, state_max, state_norm, state)


def branch_kernel(
    n, gated_ref, resid_ref, table_ref, gains_ref, gate_w_ref, mix_hbm,
    eg_hbm, eu_hbm, ed_hbm, dg_hbm, du_hbm, dd_hbm, out_ref,
    middle, mix, rows, eg, eu, ed, dg, du, dd, hid_e, hid_d,
    term, recv1, part1, recv2, part2, recv3,
    load, send_z, send_y, send_d, recv, s1, r1, s2, r2, s3, r3,
):
    groups = n // 4
    a, b, c = place()
    me = lax.axis_index("ep")
    rows_local, d = resid_ref.shape
    experts_local = eg.shape[0]
    order = near_first(groups)
    y_peer, d_peer = device(a, 1 - b, c), device(a, b, 1 - c)
    barrier = pltpu.get_barrier_semaphore()
    for to in [device(lax.rem(a + k, groups), b, c) for k in order] + [y_peer, d_peer]:
        pl.semaphore_signal(barrier, inc=1, device_id=to, device_id_type=MESH)
    loads = []
    for i, (src, dst) in enumerate(
        ((mix_hbm, mix), (dg_hbm, dg), (du_hbm, du), (eg_hbm, eg), (eu_hbm, eu), (dd_hbm, dd), (ed_hbm, ed))
    ):
        loads.append(pltpu.make_async_copy(src, dst, load.at[i]))
        loads[-1].start()
    rows[c, b, a] = jnp.zeros(rows.shape[3:], BF16)
    loads[0].wait()
    mixed = jnp.dot(gated_ref[...], mix[...], preferred_element_type=F32)
    stream = resid_ref[...].astype(F32) + rms_scale(mixed, gains_ref[1:2, :])
    middle[...] = stream
    lanes_all = table_ref.shape[1]
    rows[c, b, a, 0:rows_local, 0:d] = rms_scale(stream, gains_ref[2:3, :]).astype(BF16)
    rows[c, b, a, 0:rows_local, d : d + lanes_all] = table_ref[...]
    pl.semaphore_wait(barrier, groups + 1)
    gather(rows, a, b, c, groups, send_z, send_y, send_d, recv)
    for copy in loads[1:]:
        copy.wait()

    everything = rows[:, :, :, :, 0:d].reshape(n * ROWS, d)
    table = rows[:, :, :, :, d : d + lanes_all].reshape(n * ROWS, lanes_all).astype(F32)
    total = jnp.sum(table, axis=-1, keepdims=True)
    total = jnp.where(total > 0.0, total, 1.0)
    lanes = lax.broadcasted_iota(jnp.int32, table.shape, 1)
    logit = jnp.sum(everything.astype(F32) * gate_w_ref[...].astype(F32), axis=-1, keepdims=True)
    branch_gate = jax.nn.sigmoid(logit)

    def ffn(gate, up, hid, wide):
        step = min(256, wide)
        for j in range(wide // step):
            cols = slice(j * step, (j + 1) * step)
            g = jnp.dot(everything, gate[:, cols], preferred_element_type=F32)
            u = jnp.dot(everything, up[:, cols], preferred_element_type=F32)
            hid[:, cols] = (jax.nn.silu(g) * u).astype(BF16)

    ffn(dg, du, hid_d, dg.shape[1])
    shares = []
    for e in range(experts_local):
        ffn(eg.at[e], eu.at[e], hid_e.at[e], eg.shape[2])
        mine = jnp.sum(jnp.where(lanes == me * experts_local + e, table, 0.0), axis=-1, keepdims=True)
        shares.append(mine / total)

    wide = d // CHUNKS
    copies = []
    for h in range(CHUNKS):
        cols = slice(h * wide, (h + 1) * wide)
        value = (jnp.dot(hid_d[...], dd[:, cols], preferred_element_type=F32) * branch_gate).astype(BF16).astype(F32)
        for e in range(experts_local):
            y = jnp.dot(hid_e[e], ed[e, :, cols], preferred_element_type=F32).astype(BF16).astype(F32)
            value = value + (shares[e] * y).astype(BF16).astype(F32)
        term[h] = value.astype(BF16).reshape(2, 2, groups, ROWS, wide)
        copies.append(push(term.at[h, 1 - c], recv1.at[h], s1.at[h], r1.at[h], d_peer))
    for h in range(CHUNKS):
        copies[h].wait_recv()
        part1[h] = (term[h, c].astype(F32) + recv1[h].astype(F32)).astype(BF16)
        copies.append(push(part1.at[h, 1 - b], recv2.at[h], s2.at[h], r2.at[h], y_peer))
    for h in range(CHUNKS):
        copies[CHUNKS + h].wait_recv()
        part2[h] = (part1[h, b].astype(F32) + recv2[h].astype(F32)).astype(BF16)
        for k in order:
            to = lax.rem(a + k, groups)
            copies.append(
                push(part2.at[h, to], recv3.at[h, a], s3.at[h, k], r3.at[h, a], device(to, b, c))
            )
    sums, square = [], 0.0
    for h in range(CHUNKS):
        value = part2[h, a].astype(F32)
        for k in order:
            src = lax.rem(a + k, groups)
            arrived(recv3.at[h, src], s3.at[h, k], r3.at[h, src], device(src, b, c))
            value = value + recv3[h, src].astype(F32)
        sums.append(value)
        square = square + jnp.sum(value * value, axis=-1, keepdims=True)
    scale = lax.rsqrt(square / d + 1e-06)
    for h in range(CHUNKS):
        cols = slice(h * wide, (h + 1) * wide)
        extra = (sums[h] * scale * gains_ref[3:4, cols])[0:rows_local]
        out_ref[:, cols] = (middle[:, cols] + extra).astype(BF16)
    for copy in copies:
        copy.wait_send()


def branches(gated, resid, table, gains, gate_w, w_mix, experts, dense, n):
    rows_local, d = resid.shape
    groups = n // 4
    vmem = pl.BlockSpec(memory_space=pltpu.VMEM)
    hbm = pl.BlockSpec(memory_space=pltpu.HBM)
    wide = d // CHUNKS
    dma = pltpu.SemaphoreType.DMA
    return pl.pallas_call(
        functools.partial(branch_kernel, n),
        out_shape=jax.ShapeDtypeStruct((rows_local, d), BF16),
        in_specs=[vmem] * 5 + [hbm] * 7,
        out_specs=vmem,
        scratch_shapes=[
            pltpu.VMEM((rows_local, d), F32),
            pltpu.VMEM(w_mix.shape, BF16),
            pltpu.VMEM((2, 2, groups, ROWS, d + table.shape[1]), BF16),
            *[pltpu.VMEM(w.shape, BF16) for w in experts],
            *[pltpu.VMEM(w.shape, BF16) for w in dense],
            pltpu.VMEM((experts[0].shape[0], n * ROWS, experts[0].shape[2]), BF16),
            pltpu.VMEM((n * ROWS, dense[0].shape[1]), BF16),
            pltpu.VMEM((CHUNKS, 2, 2, groups, ROWS, wide), BF16),
            pltpu.VMEM((CHUNKS, 2, groups, ROWS, wide), BF16),
            pltpu.VMEM((CHUNKS, 2, groups, ROWS, wide), BF16),
            pltpu.VMEM((CHUNKS, groups, ROWS, wide), BF16),
            pltpu.VMEM((CHUNKS, groups, ROWS, wide), BF16),
            pltpu.VMEM((CHUNKS, groups, ROWS, wide), BF16),
            dma((7,)),
            dma((groups,)),
            dma((groups,)),
            dma((2, groups)),
            dma((2, 2, groups)),
            dma((CHUNKS,)),
            dma((CHUNKS,)),
            dma((CHUNKS,)),
            dma((CHUNKS,)),
            dma((CHUNKS, groups)),
            dma((CHUNKS, groups)),
        ],
        compiler_params=pltpu.CompilerParams(
            collective_id=1, has_side_effects=True, vmem_limit_bytes=VMEM_BYTES
        ),
        cost_estimate=spent(25),
        name="branches",
    )(gated, resid, table, gains, gate_w, w_mix, *experts, *dense)


def local(
    resid, norm_gains, w_query, w_key, w_value, w_outgate, w_igate, w_fgate,
    igate_bias, fgate_bias, state_matrix, state_norm, state_max, w_mix_out,
    routes, route_scores, expert_gate, expert_up, expert_down,
    dense_gate, dense_up, dense_down, branch_weight,
):
    devices_ep = lax.axis_size("ep")
    proj = project(
        resid, norm_gains[0:1], (w_query.T, w_key.T, w_value.T, w_outgate.T), devices_ep
    )
    new_matrix, new_norm, new_max, gated = cell_update(
        proj, resid, norm_gains[0:1], (w_igate.T, w_fgate.T),
        (igate_bias[None], fgate_bias[None]), state_max, state_norm, state_matrix,
    )
    experts = expert_gate.shape[0] * devices_ep
    lanes = jnp.arange(-(-experts // TABLE) * TABLE, dtype=jnp.int32)
    table = jnp.sum(
        jnp.where(routes[:, :, None] == lanes, route_scores.astype(F32)[:, :, None], 0.0), axis=1
    ).astype(BF16)
    out_stream = branches(
        gated, resid, table, norm_gains, branch_weight[None], w_mix_out,
        (expert_gate, expert_up, expert_down), (dense_gate, dense_up, dense_down), devices_ep,
    )
    return (out_stream, new_matrix, new_norm, new_max)


def solution(mesh):
    rows = ("grp", "ep")
    placed = (
        P(rows, None),
        P(),
        P(None, "ep"),
        P(None, "ep"),
        P(None, "ep"),
        P(None, "ep"),
        P(),
        P(),
        P(),
        P(),
        P(rows, None, None, None),
        P(rows, None, None),
        P(rows, None),
        P(),
        P(rows, None),
        P(rows, None),
        P("ep", None, None),
        P("ep", None, None),
        P("ep", None, None),
        P(None, "ep"),
        P(None, "ep"),
        P("ep", None),
        P(),
    )
    return jax.shard_map(
        local,
        mesh=mesh,
        in_specs=placed,
        out_specs=(
            P(rows, None),
            P(rows, None, None, None),
            P(rows, None, None),
            P(rows, None),
        ),
        check_vma=False,
    )
```

```python
import functools

import jax
import jax.numpy as jnp
from jax import lax
from jax.experimental import pallas as pl
from jax.experimental.pallas import tpu as pltpu
from jax.sharding import PartitionSpec as P

MESH = pl.DeviceIdType.MESH
F32 = jnp.float32
BF16 = jnp.bfloat16
ROWS = 16
TABLE = 128
VMEM_BYTES = 61 * 2**20
CHUNKS = 4


def rms_scale(values, gains):
    return values * lax.rsqrt(jnp.mean(values * values, axis=-1, keepdims=True) + 1e-06) * gains


def spent(us):
    return pl.CostEstimate(flops=us * 10**9, bytes_accessed=us * 2 * 10**6, transcendentals=0)


def dot_t(left, right):
    return lax.dot_general(left, right, (((1,), (1,)), ((), ())), preferred_element_type=F32)


def place():
    me = lax.axis_index("ep")
    return lax.div(me, 4), lax.rem(lax.div(me, 2), 2), lax.rem(me, 2)


def device(a, b, c):
    return {"ep": (a * 2 + b) * 2 + c}


def near_first(count):
    return sorted(range(1, count), key=lambda k: (min(k, count - k), k))


def push(src, dst, send_sem, recv_sem, to):
    copy = pltpu.make_async_remote_copy(
        src_ref=src, dst_ref=dst, send_sem=send_sem, recv_sem=recv_sem,
        device_id=to, device_id_type=MESH,
    )
    copy.start()
    return copy


def arrived(dst, send_sem, recv_sem, to):
    pltpu.make_async_remote_copy(
        src_ref=dst, dst_ref=dst, send_sem=send_sem, recv_sem=recv_sem,
        device_id=to, device_id_type=MESH,
    ).wait_recv()


def gather(buf, a, b, c, groups, send_z, send_y, send_d, recv):
    order = near_first(groups)
    y_peer, d_peer = device(a, 1 - b, c), device(a, b, 1 - c)
    sent = []

    def send(bb, aa, to, sem):
        block = buf.at[c, bb, aa]
        sent.append(push(block, block, sem, recv.at[c, bb, aa], to))

    def wait(cc, bb, aa):
        arrived(buf.at[cc, bb, aa], send_d.at[0, 0], recv.at[cc, bb, aa], d_peer)

    for k in order:
        send(b, a, device(lax.rem(a + k, groups), b, c), send_z.at[k])
    send(b, a, y_peer, send_y.at[0])
    send(b, a, d_peer, send_d.at[0, 0])
    for k in order:
        src = lax.rem(a + k, groups)
        wait(c, b, src)
        send(b, src, y_peer, send_y.at[k])
        send(b, src, d_peer, send_d.at[0, k])
    for k in [0] + order:
        src = lax.rem(a + k, groups)
        wait(c, 1 - b, src)
        send(1 - b, src, d_peer, send_d.at[1, k])
    for bb in range(2):
        for aa in range(groups):
            wait(1 - c, bb, aa)
    for copy in sent:
        copy.wait_send()


def project_kernel(
    n, resid_ref, gain_ref, wq_ref, wk_ref, wv_ref, wo_ref, out_ref,
    wq, wk, wv, wo, rows, local, landed, load, send_z, send_y, send_d, recv, send_x, recv_x,
):
    groups = n // 4
    a, b, c = place()
    me = lax.axis_index("ep")
    rows_local = resid_ref.shape[0]
    width = wq.shape[0]
    barrier = pltpu.get_barrier_semaphore()
    for k in range(1, n):
        pl.semaphore_signal(
            barrier, inc=1, device_id={"ep": lax.rem(me + k, n)}, device_id_type=MESH
        )
    loads = [
        pltpu.make_async_copy(src, dst, load.at[i])
        for i, (src, dst) in enumerate(((wq_ref, wq), (wk_ref, wk), (wv_ref, wv), (wo_ref, wo)))
    ]
    for copy in loads:
        copy.start()
    normed = rms_scale(resid_ref[...].astype(F32), gain_ref[...]).astype(BF16)
    rows[c, b, a] = jnp.zeros(rows.shape[3:], BF16)
    rows[c, b, a, 0:rows_local, :] = normed
    pl.semaphore_wait(barrier, n - 1)
    gather(rows, a, b, c, groups, send_z, send_y, send_d, recv)
    everything = rows[...].reshape(n * ROWS, rows.shape[-1])
    for copy in loads:
        copy.wait()
    for m, w_ref in enumerate((wq, wk, wv, wo)):
        piece = dot_t(everything, w_ref[...]).astype(BF16)
        local[:, :, :, :, m * width : (m + 1) * width] = piece.reshape(2, 2, groups, ROWS, width)
    sent = []
    for k in range(1, n):
        to = lax.rem(me + k, n)
        block = local.at[lax.rem(to, 2), lax.rem(lax.div(to, 2), 2), lax.div(to, 4)]
        sent.append(push(block, landed.at[c, b, a], send_x.at[k], recv_x.at[c, b, a], {"ep": to}))
    landed[c, b, a] = local[c, b, a]
    for k in range(1, n):
        src = lax.rem(me + k, n)
        cc, bb, aa = lax.rem(src, 2), lax.rem(lax.div(src, 2), 2), lax.div(src, 4)
        arrived(landed.at[cc, bb, aa], send_x.at[k], recv_x.at[cc, bb, aa], {"ep": src})
    for aa in range(groups):
        for bb in range(2):
            for cc in range(2):
                start = ((aa * 2 + bb) * 2 + cc) * width
                for m in range(4):
                    out_ref[m, :, start : start + width] = landed[
                        cc, bb, aa, :, m * width : (m + 1) * width
                    ]
    for copy in sent:
        copy.wait_send()


def project(resid, gain, weights, n):
    rows_local, d = resid.shape
    width = weights[0].shape[0]
    groups = n // 4
    vmem = pl.BlockSpec(memory_space=pltpu.VMEM)
    return pl.pallas_call(
        functools.partial(project_kernel, n),
        out_shape=jax.ShapeDtypeStruct((4, ROWS, n * width), BF16),
        in_specs=[vmem] * 2 + [pl.BlockSpec(memory_space=pltpu.HBM)] * 4,
        out_specs=vmem,
        scratch_shapes=[
            *[pltpu.VMEM(w.shape, BF16) for w in weights],
            pltpu.VMEM((2, 2, groups, ROWS, d), BF16),
            pltpu.VMEM((2, 2, groups, ROWS, 4 * width), BF16),
            pltpu.VMEM((2, 2, groups, ROWS, 4 * width), BF16),
            pltpu.SemaphoreType.DMA((4,)),
            pltpu.SemaphoreType.DMA((groups,)),
            pltpu.SemaphoreType.DMA((groups,)),
            pltpu.SemaphoreType.DMA((2, groups)),
            pltpu.SemaphoreType.DMA((2, 2, groups)),
            pltpu.SemaphoreType.DMA((n,)),
            pltpu.SemaphoreType.DMA((2, 2, groups)),
        ],
        compiler_params=pltpu.CompilerParams(
            collective_id=0, has_side_effects=True, vmem_limit_bytes=VMEM_BYTES
        ),
        cost_estimate=spent(20),
        name="project",
    )(resid, gain, *weights)


def cell_kernel(
    proj_ref, resid_ref, gain_ref, wi_ref, wf_ref, bi_ref, bf_ref, max_ref, norm_ref, state_hbm,
    matrix_hbm, norm_out, max_out, gated_ref,
    old, fresh, q3, k3, wv3, keep3, numer3, load, sem,
):
    count, heads, size, _ = old.shape

    def loading(s):
        return pltpu.make_async_copy(state_hbm.at[s], old.at[s], load.at[s])

    for s in range(count):
        loading(s).start()
    normed = rms_scale(resid_ref[...].astype(F32), gain_ref[...]).astype(BF16)
    ipre = dot_t(normed, wi_ref[...]) + bi_ref[...]
    fpre = dot_t(normed, wf_ref[...]) + bf_ref[...]
    logf = jnp.minimum(fpre, 0.0) - jnp.log1p(jnp.exp(-jnp.abs(fpre)))
    old_max = logf + max_ref[...]
    new_max = jnp.maximum(ipre, old_max)
    max_out[...] = new_max
    keep = jnp.exp(old_max - new_max)
    write = jnp.exp(ipre - new_max)
    denoms = []
    for h in range(heads):
        cols = slice(h * size, (h + 1) * size)
        q = proj_ref[0, 0:count, cols].astype(F32)
        k = proj_ref[1, 0:count, cols].astype(F32) * size ** (-0.5)
        v = proj_ref[2, 0:count, cols].astype(F32)
        keep_h, write_h = keep[:, h : h + 1], write[:, h : h + 1]
        new_norm = keep_h * norm_ref[:, h, :] + write_h * k
        norm_out[:, h, :] = new_norm
        denoms.append(jnp.maximum(jnp.abs(jnp.sum(new_norm * q, axis=-1, keepdims=True)), 1.0))
        q3[:, h, :] = q
        k3[:, h, :] = k
        wv3[:, h, :] = write_h * v
        keep3[:, h, :] = jnp.broadcast_to(keep_h, (count, size))

    def sequence(s, carry):
        q, k, kept = q3[s], k3[s], keep3[s]
        loading(s).wait()
        column = wv3[s].T
        row = lax.broadcasted_iota(jnp.int32, (heads, size), 0)
        numer = jnp.zeros((heads, size), F32)
        q = q.astype(BF16)
        for h in range(heads):
            new = (
                old[s, h] * kept[h : h + 1, :] + column[:, h : h + 1] * k[h : h + 1, :]
            )
            fresh[s, h] = new
            high = new.astype(BF16)
            low = (new - high.astype(F32)).astype(BF16)
            numer = jnp.where(row == h, dot_t(q, high) + dot_t(q, low), numer)
        pltpu.make_async_copy(fresh.at[s], matrix_hbm.at[s], sem.at[s]).start()
        numer3[s] = numer
        return carry

    lax.fori_loop(0, count, sequence, 0)
    for h in range(heads):
        cols = slice(h * size, (h + 1) * size)
        outgate = proj_ref[3, 0:count, cols].astype(F32)
        cell = numer3[:, h, :] / denoms[h]
        gated_ref[:, cols] = (jax.nn.sigmoid(outgate) * cell).astype(BF16)
    for s in range(count):
        pltpu.make_async_copy(fresh.at[s], matrix_hbm.at[s], sem.at[s]).wait()


def cell_update(proj, resid, gain, gates, biases, state_max, state_norm, state):
    count, heads, size, _ = state.shape
    vmem = pl.BlockSpec(memory_space=pltpu.VMEM)
    small = pltpu.VMEM((count, heads, size), F32)
    return pl.pallas_call(
        cell_kernel,
        out_shape=(
            jax.ShapeDtypeStruct(state.shape, F32),
            jax.ShapeDtypeStruct(state_norm.shape, F32),
            jax.ShapeDtypeStruct(state_max.shape, F32),
            jax.ShapeDtypeStruct((count, heads * size), BF16),
        ),
        in_specs=[vmem] * 9 + [pl.BlockSpec(memory_space=pl.ANY)],
        out_specs=(pl.BlockSpec(memory_space=pl.ANY), vmem, vmem, vmem),
        scratch_shapes=[
            pltpu.VMEM(state.shape, F32),
            pltpu.VMEM(state.shape, F32),
            small, small, small, small, small,
            pltpu.SemaphoreType.DMA((count,)),
            pltpu.SemaphoreType.DMA((count,)),
        ],
        compiler_params=pltpu.CompilerParams(vmem_limit_bytes=VMEM_BYTES),
        cost_estimate=spent(6),
        name="cell_update",
    )(proj, resid, gain, *gates, *biases, state_max, state_norm, state)


def branch_kernel(
    n, gated_ref, resid_ref, table_ref, gains_ref, gate_w_ref, mix_hbm,
    eg_hbm, eu_hbm, ed_hbm, dg_hbm, du_hbm, dd_hbm, out_ref,
    middle, mix, rows, eg, eu, ed, dg, du, dd, hid_e, hid_d,
    term, recv1, part1, recv2, part2, recv3,
    load, send_z, send_y, send_d, recv, s1, r1, s2, r2, s3, r3,
):
    groups = n // 4
    a, b, c = place()
    me = lax.axis_index("ep")
    rows_local, d = resid_ref.shape
    experts_local = eg.shape[0]
    order = near_first(groups)
    y_peer, d_peer = device(a, 1 - b, c), device(a, b, 1 - c)
    barrier = pltpu.get_barrier_semaphore()
    for to in [device(lax.rem(a + k, groups), b, c) for k in order] + [y_peer, d_peer]:
        pl.semaphore_signal(barrier, inc=1, device_id=to, device_id_type=MESH)
    loads = []
    for i, (src, dst) in enumerate(
        ((mix_hbm, mix), (dg_hbm, dg), (du_hbm, du), (eg_hbm, eg), (eu_hbm, eu), (dd_hbm, dd), (ed_hbm, ed))
    ):
        loads.append(pltpu.make_async_copy(src, dst, load.at[i]))
        loads[-1].start()
    rows[c, b, a] = jnp.zeros(rows.shape[3:], BF16)
    loads[0].wait()
    mixed = jnp.dot(gated_ref[...], mix[...], preferred_element_type=F32)
    stream = resid_ref[...].astype(F32) + rms_scale(mixed, gains_ref[1:2, :])
    middle[...] = stream
    lanes_all = table_ref.shape[1]
    rows[c, b, a, 0:rows_local, 0:d] = rms_scale(stream, gains_ref[2:3, :]).astype(BF16)
    rows[c, b, a, 0:rows_local, d : d + lanes_all] = table_ref[...]
    pl.semaphore_wait(barrier, groups + 1)
    gather(rows, a, b, c, groups, send_z, send_y, send_d, recv)
    for copy in loads[1:]:
        copy.wait()

    everything = rows[:, :, :, :, 0:d].reshape(n * ROWS, d)
    table = rows[:, :, :, :, d : d + lanes_all].reshape(n * ROWS, lanes_all).astype(F32)
    total = jnp.sum(table, axis=-1, keepdims=True)
    total = jnp.where(total > 0.0, total, 1.0)
    lanes = lax.broadcasted_iota(jnp.int32, table.shape, 1)
    logit = jnp.sum(everything.astype(F32) * gate_w_ref[...].astype(F32), axis=-1, keepdims=True)
    branch_gate = jax.nn.sigmoid(logit)

    def ffn(gate, up, hid, wide):
        step = min(256, wide)
        for j in range(wide // step):
            cols = slice(j * step, (j + 1) * step)
            g = jnp.dot(everything, gate[:, cols], preferred_element_type=F32)
            u = jnp.dot(everything, up[:, cols], preferred_element_type=F32)
            hid[:, cols] = (jax.nn.silu(g) * u).astype(BF16)

    ffn(dg, du, hid_d, dg.shape[1])
    shares = []
    for e in range(experts_local):
        ffn(eg.at[e], eu.at[e], hid_e.at[e], eg.shape[2])
        mine = jnp.sum(jnp.where(lanes == me * experts_local + e, table, 0.0), axis=-1, keepdims=True)
        shares.append(mine / total)

    wide = d // CHUNKS
    copies = []
    for h in range(CHUNKS):
        cols = slice(h * wide, (h + 1) * wide)
        value = (jnp.dot(hid_d[...], dd[:, cols], preferred_element_type=F32) * branch_gate).astype(BF16).astype(F32)
        for e in range(experts_local):
            y = jnp.dot(hid_e[e], ed[e, :, cols], preferred_element_type=F32).astype(BF16).astype(F32)
            value = value + (shares[e] * y).astype(BF16).astype(F32)
        term[h] = value.astype(BF16).reshape(2, 2, groups, ROWS, wide)
        copies.append(push(term.at[h, 1 - c], recv1.at[h], s1.at[h], r1.at[h], d_peer))
    for h in range(CHUNKS):
        copies[h].wait_recv()
        part1[h] = (term[h, c].astype(F32) + recv1[h].astype(F32)).astype(BF16)
        copies.append(push(part1.at[h, 1 - b], recv2.at[h], s2.at[h], r2.at[h], y_peer))
    for h in range(CHUNKS):
        copies[CHUNKS + h].wait_recv()
        part2[h] = (part1[h, b].astype(F32) + recv2[h].astype(F32)).astype(BF16)
        for k in order:
            to = lax.rem(a + k, groups)
            copies.append(
                push(part2.at[h, to], recv3.at[h, a], s3.at[h, k], r3.at[h, a], device(to, b, c))
            )
    sums, square = [], 0.0
    for h in range(CHUNKS):
        value = part2[h, a].astype(F32)
        for k in order:
            src = lax.rem(a + k, groups)
            arrived(recv3.at[h, src], s3.at[h, k], r3.at[h, src], device(src, b, c))
            value = value + recv3[h, src].astype(F32)
        sums.append(value)
        square = square + jnp.sum(value * value, axis=-1, keepdims=True)
    scale = lax.rsqrt(square / d + 1e-06)
    for h in range(CHUNKS):
        cols = slice(h * wide, (h + 1) * wide)
        extra = (sums[h] * scale * gains_ref[3:4, cols])[0:rows_local]
        out_ref[:, cols] = (middle[:, cols] + extra).astype(BF16)
    for copy in copies:
        copy.wait_send()


def branches(gated, resid, table, gains, gate_w, w_mix, experts, dense, n):
    rows_local, d = resid.shape
    groups = n // 4
    vmem = pl.BlockSpec(memory_space=pltpu.VMEM)
    hbm = pl.BlockSpec(memory_space=pltpu.HBM)
    wide = d // CHUNKS
    dma = pltpu.SemaphoreType.DMA
    return pl.pallas_call(
        functools.partial(branch_kernel, n),
        out_shape=jax.ShapeDtypeStruct((rows_local, d), BF16),
        in_specs=[vmem] * 5 + [hbm] * 7,
        out_specs=vmem,
        scratch_shapes=[
            pltpu.VMEM((rows_local, d), F32),
            pltpu.VMEM(w_mix.shape, BF16),
            pltpu.VMEM((2, 2, groups, ROWS, d + table.shape[1]), BF16),
            *[pltpu.VMEM(w.shape, BF16) for w in experts],
            *[pltpu.VMEM(w.shape, BF16) for w in dense],
            pltpu.VMEM((experts[0].shape[0], n * ROWS, experts[0].shape[2]), BF16),
            pltpu.VMEM((n * ROWS, dense[0].shape[1]), BF16),
            pltpu.VMEM((CHUNKS, 2, 2, groups, ROWS, wide), BF16),
            pltpu.VMEM((CHUNKS, 2, groups, ROWS, wide), BF16),
            pltpu.VMEM((CHUNKS, 2, groups, ROWS, wide), BF16),
            pltpu.VMEM((CHUNKS, groups, ROWS, wide), BF16),
            pltpu.VMEM((CHUNKS, groups, ROWS, wide), BF16),
            pltpu.VMEM((CHUNKS, groups, ROWS, wide), BF16),
            dma((7,)),
            dma((groups,)),
            dma((groups,)),
            dma((2, groups)),
            dma((2, 2, groups)),
            dma((CHUNKS,)),
            dma((CHUNKS,)),
            dma((CHUNKS,)),
            dma((CHUNKS,)),
            dma((CHUNKS, groups)),
            dma((CHUNKS, groups)),
        ],
        compiler_params=pltpu.CompilerParams(
            collective_id=1, has_side_effects=True, vmem_limit_bytes=VMEM_BYTES
        ),
        cost_estimate=spent(25),
        name="branches",
    )(gated, resid, table, gains, gate_w, w_mix, *experts, *dense)


def local(
    resid, norm_gains, w_query, w_key, w_value, w_outgate, w_igate, w_fgate,
    igate_bias, fgate_bias, state_matrix, state_norm, state_max, w_mix_out,
    routes, route_scores, expert_gate, expert_up, expert_down,
    dense_gate, dense_up, dense_down, branch_weight,
):
    devices_ep = lax.axis_size("ep")
    proj = project(
        resid, norm_gains[0:1], (w_query.T, w_key.T, w_value.T, w_outgate.T), devices_ep
    )
    new_matrix, new_norm, new_max, gated = cell_update(
        proj, resid, norm_gains[0:1], (w_igate.T, w_fgate.T),
        (igate_bias[None], fgate_bias[None]), state_max, state_norm, state_matrix,
    )
    experts = expert_gate.shape[0] * devices_ep
    lanes = jnp.arange(-(-experts // TABLE) * TABLE, dtype=jnp.int32)
    table = jnp.sum(
        jnp.where(routes[:, :, None] == lanes, route_scores.astype(F32)[:, :, None], 0.0), axis=1
    ).astype(BF16)
    out_stream = branches(
        gated, resid, table, norm_gains, branch_weight[None], w_mix_out,
        (expert_gate, expert_up, expert_down), (dense_gate, dense_up, dense_down), devices_ep,
    )
    return (out_stream, new_matrix, new_norm, new_max)


def solution(mesh):
    rows = ("grp", "ep")
    placed = (
        P(rows, None),
        P(),
        P(None, "ep"),
        P(None, "ep"),
        P(None, "ep"),
        P(None, "ep"),
        P(),
        P(),
        P(),
        P(),
        P(rows, None, None, None),
        P(rows, None, None),
        P(rows, None),
        P(),
        P(rows, None),
        P(rows, None),
        P("ep", None, None),
        P("ep", None, None),
        P("ep", None, None),
        P(None, "ep"),
        P(None, "ep"),
        P("ep", None),
        P(),
    )
    return jax.shard_map(
        local,
        mesh=mesh,
        in_specs=placed,
        out_specs=(
            P(rows, None),
            P(rows, None, None, None),
            P(rows, None, None),
            P(rows, None),
        ),
        check_vma=False,
    )
```
